32 devices in a mesh: ep: 8 (over z, x), tp: 4 (over y, core).
Axes of the slice: x: 2, y: 2, z: 4, core: 2. Of those that a mesh axis runs over, the one named last changes fastest.
Arguments:
- tokens: bfloat16 [128, 1024], P('ep'), may hold values from -6 to 6
- memory: float32 [128, 4, 128, 256], P('ep', 'tp'), may hold values from -6 to 6
- log_scale: float32 [128, 4], P('ep', 'tp'), may hold values from -1 to 130
- mix_gain_in: float32 [1024], replicated, may hold values from 0.1 to 1.9
- w_query: bfloat16 [1024, 512], P(None, 'tp'), may hold values from -0.1875 to 0.1875
- w_key: bfloat16 [1024, 512], P(None, 'tp'), may hold values from -0.1875 to 0.1875
- w_value: bfloat16 [1024, 1024], P(None, 'tp'), may hold values from -0.1875 to 0.1875
- w_igate: bfloat16 [1024, 4], P(None, 'tp'), may hold values from -0.1875 to 0.1875
- w_fgate: bfloat16 [1024, 4], P(None, 'tp'), may hold values from -0.1875 to 0.1875
- igate_bias: float32 [4], P('tp'), may hold values from -1 to 1
- fgate_bias: float32 [4], P('tp'), may hold values from 0 to 4
- head_gain: float32 [1024], P('tp'), may hold values from 0.1 to 1.9
- w_output: bfloat16 [1024, 1024], P('tp'), may hold values from -0.1875 to 0.1875
- mix_gain_out: float32 [1024], replicated, may hold values from 0.1 to 1.9
- ffn_gain_in: float32 [1024], replicated, may hold values from 0.1 to 1.9
- routes: int32 [128, 6], P('ep'), may hold values from 0 to 7, all different within a row; in each aligned block of 16 rows (0 to 15, 16 to 31, ...) at most 16 rows name the same one
- route_weights: float32 [128, 6], P('ep'), may hold values from 0.1 to 1
- expert_gate: bfloat16 [8, 1024, 1024], P('ep', None, 'tp'), may hold values from -0.1875 to 0.1875
- expert_up: bfloat16 [8, 1024, 1024], P('ep', None, 'tp'), may hold values from -0.1875 to 0.1875
- expert_down: bfloat16 [8, 1024, 1024], P('ep', 'tp'), may hold values from -0.9375 to 0.9375
- ffn_gain_out: float32 [1024], P('tp'), may hold values from 0.1 to 1.9
Outputs:
- output: bfloat16 [128, 1024], P('ep', 'tp')
The draws below stay inside these ranges and needn't reach their ends.
Inputs may be any that keep to these rules, and one draw needn't show every extreme that they name: `routes`: among the 16 tokens of one index of ep no expert is named by more than 16 tokens, and in every draw some expert is named by exactly 16 of them.
All inputs are finite; a program needn't handle non-finite values.
Results may differ from the reference program's by a relative error of at most 0.02.
Values may be sent and summed in bfloat16 or wider, within the bound.
A program may use at most 64 MiB of HBM per device.

```python
import math
import jax
import jax.numpy as jnp
import numpy as np
from jax import lax

D = 1024
HEADS = 4
KEY_DIM = 128
VALUE_DIM = 256
EXPERT_WIDTH = 1024
TOP_K = 6
SEQ_G = 16
EXPERTS = 8
CAP = 16
BATCH = 128
N_EP = 8


def draw_log_scale(key, part):
    base_key = jax.random.fold_in(key, 11)
    values = jax.random.uniform(base_key, (BATCH, HEADS), jnp.float32, -1.0, 3.0)
    return values


def draw_expert_down(key, part):
    noise_key = jax.random.fold_in(key, 21)
    column_key = jax.random.fold_in(key, 22)
    raw = jnp.clip(jax.random.normal(noise_key, (EXPERTS, EXPERT_WIDTH, D), jnp.float32), -4.0, 4.0)
    spot = (jnp.arange(D, dtype=jnp.float32) + 0.5) / D
    jitter = jax.random.uniform(column_key, (D,), jnp.float32, -0.4, 0.4)
    ramp = 1.2 * (2.0 * spot - 1.0)
    scale = jnp.exp(ramp + jitter) * EXPERT_WIDTH ** (-0.5)
    return (raw * scale[None, None, :]).astype(jnp.bfloat16)


def block_scale(stream_key, dims, pieces, smallest, largest):
    loudness, own = 1.0, jax.random.fold_in(stream_key, 6)
    for dim, parts in pieces:
        heights = jnp.exp(jax.random.uniform(jax.random.fold_in(own, dim), (parts,), jnp.float32, smallest / len(pieces), largest / len(pieces)))
        loudness = loudness * jnp.repeat(heights, dims[dim] // parts).reshape([-1 if axis == dim else 1 for axis in range(len(dims))])
    return loudness


def assign_block(rng, own, number, rows, number_of, top, reach, lean):
    ranking = jax.random.permutation(rng, number_of)
    crowded, usual = portions_of(number_of, rows * top, reach, lean, True), portions_of(number_of, rows * top, reach, lean, False)
    places = jnp.arange(number_of)

    def named(sizes, turn):
        used = int((sizes > 0).sum())
        fixed = max(1, used // 4)
        moved = fixed + (places - fixed + turn * (used - fixed)) % max(1, number_of - fixed)
        return jnp.zeros((number_of,), jnp.int32).at[ranking[jnp.where(places < fixed, places, moved)]].set(jnp.asarray(sizes, jnp.int32))

    sizes = jnp.where(number % 4 == 0, named(crowded, number // 4), named(usual, number - number // 4 - 1))
    mixed = jax.random.permutation(jax.random.fold_in(own, 3), number_of)
    giver, taker = mixed[0:number_of // 2 * 2:2], mixed[1:number_of // 2 * 2:2]
    slack = jnp.minimum(sizes[giver] - 1, reach - sizes[taker]) // 2
    slack = jnp.where((giver == ranking[0]) | (taker == ranking[0]) | (sizes[taker] == 0), 0, jnp.maximum(slack, 0))
    moved = jax.random.randint(jax.random.fold_in(own, 4), (number_of // 2,), 0, 1 << 20) % (slack + 1)
    sizes = sizes.at[giver].add(-moved).at[taker].add(moved)
    members = jnp.searchsorted(jnp.cumsum(sizes), jnp.arange(rows * top), side="right").astype(jnp.int32)
    listing = members.reshape(top, rows).T
    listing = listing[jax.random.permutation(jax.random.fold_in(own, 1), rows)]
    turn = jax.random.randint(jax.random.fold_in(own, 2), (rows, 1), 0, top)
    return jnp.take_along_axis(listing, (jnp.arange(top)[None, :] + turn) % top, axis=1)


def portions_of(number_of, total, reach, lean, full):
    portions = [(1 << 20) // math.isqrt(rank ** lean) + 1 for rank in range(1, number_of + 1)]
    largest = reach if full else min(reach, max(-(-total // number_of), total * portions[0] // sum(portions)))
    least = 1 if total - largest >= number_of - 1 else 0
    counts, rest = [largest] + [least] * (number_of - 1), total - largest - least * (number_of - 1)
    while rest > 0:
        candidates = [i for i in range(1, number_of) if counts[i] < largest] or [i for i in range(1, number_of) if counts[i] < reach]
        pool, remaining = sum([portions[i] for i in candidates]), rest
        for i in candidates:
            addition = min(reach - counts[i], max(1, remaining * portions[i] // pool), rest)
            counts[i] = counts[i] + addition
            rest = rest - addition
    return np.array(counts)


def noise(key, shape, scale, bound, split=(), held_as=jnp.bfloat16):
    values = jax.random.normal(key, shape, jnp.float32) * scale
    if len(split) > 0:
        values = block_scale(key, shape, split, -0.22, 0.18) * values
    return jnp.clip(values, min=-bound, max=bound).astype(held_as)


def setup_inputs(seed: int = 0) -> dict:
    splits = jax.random.split(jax.random.key(seed), 22)
    tokens = noise(splits[0], (BATCH, D), 1.0, 6.0, ((0, 8),))
    memory = noise(splits[1], (BATCH, HEADS, KEY_DIM, VALUE_DIM), 1.0, 6.0, ((0, 8), (1, 4)), jnp.float32)
    log_scale = draw_log_scale(jax.random.fold_in(splits[21], 71), 0)
    mix_gain_in = jnp.clip(1.0 + 0.18 * jax.random.normal(splits[3], (D,), jnp.float32), 0.1, 1.9)
    w_query = noise(splits[4], (D, HEADS * KEY_DIM), D ** -0.5, 0.1875, ((1, 4),))
    w_key = noise(splits[5], (D, HEADS * KEY_DIM), D ** -0.5, 0.1875, ((1, 4),))
    w_value = noise(splits[6], (D, HEADS * VALUE_DIM), D ** -0.5, 0.1875, ((1, 4),))
    w_igate = noise(splits[7], (D, HEADS), D ** -0.5, 0.1875, ((1, 4),))
    w_fgate = noise(splits[8], (D, HEADS), D ** -0.5, 0.1875, ((1, 4),))
    igate_bias = jnp.clip(jax.random.uniform(splits[9], (HEADS,), jnp.float32, -1.0, 1.0) * block_scale(splits[9], (HEADS,), ((0, 4),), -0.4, 0.0), -1.0, 1.0)
    fgate_bias = jnp.clip(4.0 * jax.random.uniform(splits[10], (HEADS,), jnp.float32) ** block_scale(splits[10], (HEADS,), ((0, 4),), -0.2, 0.2), 0.0, 4.0)
    head_gain = jnp.clip(1.0 + 0.18 * jax.random.normal(splits[11], (HEADS * VALUE_DIM,), jnp.float32), 0.1, 1.9)
    w_output = noise(splits[12], (HEADS * VALUE_DIM, D), (HEADS * VALUE_DIM) ** -0.5, 0.1875, ((0, 4),))
    mix_gain_out = jnp.clip(1.0 + 0.18 * jax.random.normal(splits[13], (D,), jnp.float32), 0.1, 1.9)
    ffn_gain_in = jnp.clip(1.0 + 0.18 * jax.random.normal(splits[14], (D,), jnp.float32), 0.1, 1.9)
    routes_keys = jax.random.split(jax.random.fold_in(splits[15], 1), BATCH // SEQ_G)
    routes_turns = jax.random.permutation(jax.random.fold_in(splits[15], 3), BATCH // SEQ_G)
    routes = jax.vmap(lambda own, number: assign_block(jax.random.fold_in(splits[15], 2), own, number, SEQ_G, EXPERTS, TOP_K, CAP, 1))(routes_keys, routes_turns).reshape((BATCH, TOP_K))
    route_weights = jnp.clip(jnp.exp(math.log(1.0) - 2.3025851 * jax.random.uniform(splits[16], (BATCH, TOP_K), jnp.float32) ** block_scale(splits[16], (BATCH, TOP_K), ((0, 8),), -0.2, 0.2)), 0.1, 1.0)
    expert_gate = noise(splits[17], (EXPERTS, D, EXPERT_WIDTH), D ** -0.5, 0.1875, ((0, 8), (2, 4)))
    expert_up = noise(splits[18], (EXPERTS, D, EXPERT_WIDTH), D ** -0.5, 0.1875, ((0, 8), (2, 4)))
    expert_down = draw_expert_down(jax.random.fold_in(splits[21], 71), 0)
    ffn_gain_out = jnp.clip(1.0 + 0.18 * jax.random.normal(splits[20], (D,), jnp.float32), 0.1, 1.9)
    return dict(tokens=tokens, memory=memory, log_scale=log_scale, mix_gain_in=mix_gain_in, w_query=w_query, w_key=w_key, w_value=w_value, w_igate=w_igate, w_fgate=w_fgate, igate_bias=igate_bias, fgate_bias=fgate_bias, head_gain=head_gain, w_output=w_output, mix_gain_out=mix_gain_out, ffn_gain_in=ffn_gain_in, routes=routes, route_weights=route_weights, expert_gate=expert_gate, expert_up=expert_up, expert_down=expert_down, ffn_gain_out=ffn_gain_out)


EPS = 1e-06

def rms_scale(values):
    return lax.rsqrt(lax.optimization_barrier(jnp.mean(values * values, axis=-1, keepdims=True)) + EPS)

def reference(tokens, memory, log_scale, mix_gain_in, w_query, w_key, w_value, w_igate, w_fgate, igate_bias, fgate_bias, head_gain, w_output, mix_gain_out, ffn_gain_in, routes, route_weights, expert_gate, expert_up, expert_down, ffn_gain_out):
    f32 = jnp.float32
    bf16 = jnp.bfloat16
    xf = tokens.astype(f32)
    normed = (xf * rms_scale(xf) * mix_gain_in).astype(bf16)
    query = jnp.dot(normed, w_query, preferred_element_type=f32).reshape(BATCH, HEADS, KEY_DIM) * KEY_DIM ** (-0.5)
    keys = jnp.dot(normed, w_key, preferred_element_type=f32).reshape(BATCH, HEADS, KEY_DIM)
    values = jnp.dot(normed, w_value, preferred_element_type=f32).reshape(BATCH, HEADS, VALUE_DIM)
    in_pre = jnp.dot(normed, w_igate, preferred_element_type=f32) + igate_bias
    forget_log = jax.nn.log_sigmoid(jnp.dot(normed, w_fgate, preferred_element_type=f32) + fgate_bias)
    carried = forget_log + log_scale
    new_max = jnp.maximum(carried, in_pre)
    carry_weight = jnp.exp(carried - new_max)
    fresh_weight = jnp.exp(in_pre - new_max)
    recall = jnp.einsum('bhk,bhkv->bhv', query, memory, precision=lax.Precision.HIGHEST)
    match = lax.optimization_barrier(jnp.sum(query * keys, axis=-1))
    read = carry_weight[..., None] * recall + (fresh_weight * match)[..., None] * values
    headout = (read * rms_scale(read) * head_gain.reshape(HEADS, VALUE_DIM)).astype(bf16)
    per_head = jnp.einsum('bhv,hvd->bhd', headout.astype(f32), w_output.reshape(HEADS, VALUE_DIM, D).astype(f32)).astype(bf16)
    mixed = lax.optimization_barrier(jnp.sum(per_head.astype(f32), axis=1))
    resid = (xf + mixed * rms_scale(mixed) * mix_gain_out).astype(bf16)
    rf = resid.astype(f32)
    ffn_in = (rf * rms_scale(rf) * ffn_gain_in).astype(bf16)
    rows_total = BATCH * TOP_K
    limit = N_EP * CAP
    flat = routes.reshape(-1).astype(jnp.int32)

    def per_expert(done, expert):
        found = jnp.nonzero(flat == expert, size=limit, fill_value=rows_total)[0].astype(jnp.int32)
        token = jnp.minimum(found // TOP_K, BATCH - 1)
        picked = jnp.take(ffn_in, token, axis=0)
        gate = jnp.dot(picked, expert_gate[expert], preferred_element_type=f32)
        up = jnp.dot(picked, expert_up[expert], preferred_element_type=f32)
        act = (jax.nn.silu(gate) * up).astype(bf16)
        blocks = jnp.einsum('rtf,tfd->rtd', act.reshape(limit, HEADS, EXPERT_WIDTH // HEADS).astype(f32), expert_down[expert].reshape(HEADS, EXPERT_WIDTH // HEADS, D).astype(f32)).astype(bf16)
        result = lax.optimization_barrier(jnp.sum(blocks.astype(f32), axis=1)).astype(bf16)
        done = done.at[found].set(result, mode='drop')
        return (done, None)
    done, _ = lax.scan(per_expert, jnp.zeros((rows_total, D), bf16), jnp.arange(EXPERTS, dtype=jnp.int32))
    expert_rows = done.reshape(BATCH, TOP_K, D).astype(f32)
    routed = lax.optimization_barrier(jnp.sum(route_weights[..., None] * expert_rows, axis=1))
    return (rf + routed * rms_scale(routed) * ffn_gain_out).astype(bf16)
```

```python
import functools

import jax
import jax.numpy as jnp
from jax import lax
from jax.experimental import pallas as pl
from jax.experimental.pallas import tpu as pltpu
from jax.sharding import PartitionSpec as P

EPS = 1e-06


def rms_scale(values):
    return lax.rsqrt(jnp.mean(values * values, axis=-1, keepdims=True) + EPS)


def routed_device(
    tokens,
    memory,
    log_scale,
    mix_gain_in,
    w_query,
    w_key,
    w_value,
    w_igate,
    w_fgate,
    igate_bias,
    fgate_bias,
    head_gain,
    w_output,
    mix_gain_out,
    ffn_gain_in,
    routes,
    route_weights,
    expert_gate,
    expert_up,
    expert_down,
    ffn_gain_out,
):
    f32 = jnp.float32
    bf16 = jnp.bfloat16
    seqs, width = tokens.shape
    heads = log_scale.shape[1]
    key_dim = memory.shape[2]
    value_dim = memory.shape[3]
    xf = tokens.astype(f32)
    normed = (xf * rms_scale(xf) * mix_gain_in).astype(bf16)
    query = jnp.dot(normed, w_query, preferred_element_type=f32).reshape(
        seqs, heads, key_dim
    ) * key_dim ** (-0.5)
    keys = jnp.dot(normed, w_key, preferred_element_type=f32).reshape(seqs, heads, key_dim)
    values = jnp.dot(normed, w_value, preferred_element_type=f32).reshape(seqs, heads, value_dim)
    in_pre = jnp.dot(normed, w_igate, preferred_element_type=f32) + igate_bias
    forget_log = jax.nn.log_sigmoid(
        jnp.dot(normed, w_fgate, preferred_element_type=f32) + fgate_bias
    )
    carried = forget_log + log_scale
    new_max = jnp.maximum(carried, in_pre)
    carry_weight = jnp.exp(carried - new_max)
    fresh_weight = jnp.exp(in_pre - new_max)
    recall = jnp.einsum("shk,shkv->shv", query, memory, precision=lax.Precision.HIGHEST)
    match = jnp.sum(query * keys, axis=-1)
    read = carry_weight[..., None] * recall + (fresh_weight * match)[..., None] * values
    headout = (
        (read * rms_scale(read) * head_gain.reshape(heads, value_dim))
        .astype(bf16)
        .reshape(seqs, heads * value_dim)
    )
    partial_value = jnp.dot(headout, w_output, preferred_element_type=f32)
    mixed = lax.psum(partial_value.astype(jnp.bfloat16), "tp").astype(jnp.float32)
    resid = (xf + mixed * rms_scale(mixed) * mix_gain_out).astype(bf16)
    rf = resid.astype(f32)
    ffn_in = (rf * rms_scale(rf) * ffn_gain_in).astype(bf16)
    lanes = lax.axis_size("tp")
    quarter = width // lanes
    own = lax.axis_index("tp") * quarter
    local_experts = expert_gate.shape[0]
    experts_all = local_experts * lax.axis_size("ep")
    top = routes.shape[1]
    cap = min(seqs, max(2, 3 * seqs * top // (2 * experts_all)))
    flat = routes.reshape(-1)
    hits = (flat[:, None] == jnp.arange(experts_all, dtype=jnp.int32)[None, :]).astype(jnp.int32)
    earlier = jnp.cumsum(hits, axis=0) - hits
    slot = jnp.sum(earlier * hits, axis=1)
    place = (flat * cap + slot).reshape(seqs, top)
    picker = jnp.any(
        jnp.arange(experts_all * cap, dtype=jnp.int32)[:, None, None] == place[None, :, :], axis=2
    ).astype(bf16)
    outbound = (
        jnp.dot(picker, ffn_in, preferred_element_type=f32)
        .astype(bf16)
        .reshape(experts_all, cap, width)
    )
    arrived = lax.all_to_all(outbound, "ep", split_axis=0, concat_axis=0, tiled=True)
    items = arrived.shape[1]
    rows = arrived.reshape(-1, local_experts, items, width)
    gate = jnp.einsum("secd,edf->secf", rows, expert_gate, preferred_element_type=f32)
    up = jnp.einsum("secd,edf->secf", rows, expert_up, preferred_element_type=f32)
    act = (jax.nn.silu(gate) * up).astype(bf16)
    part = jnp.einsum("secf,efd->secd", act, expert_down, preferred_element_type=f32).reshape(
        -1, items, width
    )
    summed = lax.psum_scatter(
        part.astype(jnp.bfloat16), "tp", scatter_dimension=2, tiled=True
    ).astype(jnp.float32)
    done = summed.astype(bf16)
    returned = lax.all_to_all(done, "ep", split_axis=0, concat_axis=0, tiled=True)
    columns = returned.shape[2]
    chosen = jnp.take(returned.reshape(-1, columns), place.reshape(-1), axis=0).reshape(
        seqs, top, columns
    )
    routed = jnp.sum(route_weights[:, :, None] * chosen.astype(f32), axis=1)
    resid_part = lax.dynamic_slice_in_dim(rf, own, quarter, 1)
    total = lax.psum(jnp.sum(routed * routed, axis=1), "tp")
    scaled = routed * lax.rsqrt(total / width + EPS)[:, None]
    return (resid_part + scaled * ffn_gain_out).astype(bf16)


F32 = jnp.float32
BF16 = jnp.bfloat16
MESH = pl.DeviceIdType.MESH


def column_of(row):
    n = row.shape[1]
    eye = lax.broadcasted_iota(jnp.int32, (n, n), 0) == lax.broadcasted_iota(jnp.int32, (n, n), 1)
    return jnp.sum(jnp.where(eye, jnp.broadcast_to(row, (n, n)), 0.0), axis=1, keepdims=True)


def layer_kernel(
    groups,
    lanes,
    tokens_hbm,
    memory_hbm,
    log_scale_ref,
    gain_in_ref,
    w_query_hbm,
    w_key_hbm,
    w_value_hbm,
    w_igate_ref,
    w_fgate_ref,
    igate_bias_ref,
    fgate_bias_ref,
    head_gain_ref,
    w_output_hbm,
    gain_out_ref,
    ffn_gain_ref,
    routes_ref,
    route_weights_ref,
    gate_hbm,
    up_hbm,
    down_hbm,
    ffn_gain_out_ref,
    out_ref,
    tokens_v,
    memory_v,
    w_query_v,
    w_key_v,
    w_value_v,
    w_output_v,
    gate_v,
    up_v,
    down_v,
    recall_v,
    shares,
    rows,
    resid_v,
    parts,
    results,
    squares,
    load_sem,
    memory_sem,
    share_send,
    share_recv,
    rows_send,
    rows_recv,
    parts_send,
    parts_recv,
    squares_send,
    squares_recv,
):
    ep = lax.axis_index("ep")
    tp = lax.axis_index("tp")
    seqs, width = tokens_v.shape
    key_dim = memory_v.shape[1]
    value_dim = memory_v.shape[2]
    quarter = width // lanes

    def device(off, toff):
        return (lax.rem(ep + (off % groups), groups), lax.rem(tp + (toff % lanes), lanes))

    pieces = memory_sem.shape[0]
    piece = seqs // pieces
    loads = {}
    for i, (name, src, dst) in enumerate(
        (
            ("tokens", tokens_hbm, tokens_v),
            ("query", w_query_hbm, w_query_v),
            ("key", w_key_hbm, w_key_v),
            ("value", w_value_hbm, w_value_v),
            ("output", w_output_hbm, w_output_v),
            ("gate", gate_hbm.at[0], gate_v),
            ("up", up_hbm.at[0], up_v),
            ("down", down_hbm.at[0], down_v),
        )
    ):
        loads[name] = pltpu.make_async_copy(src, dst, load_sem.at[i])
    memory_loads = [
        pltpu.make_async_copy(
            memory_hbm.at[pl.ds(i * piece, piece), 0],
            memory_v.at[pl.ds(i * piece, piece)],
            memory_sem.at[i],
        )
        for i in range(pieces)
    ]
    for name in ("tokens", "query", "key", "value"):
        loads[name].start()
    for load in memory_loads:
        load.start()
    for name in ("output", "gate", "up", "down"):
        loads[name].start()

    barrier = pltpu.get_barrier_semaphore()
    for off in range(groups):
        for toff in range(lanes):
            if off or toff:
                pl.semaphore_signal(
                    barrier, inc=1, device_id=device(off, toff), device_id_type=MESH
                )

    loads["tokens"].wait()
    xf = tokens_v[...].astype(F32)
    normed = (xf * rms_scale(xf) * gain_in_ref[...]).astype(BF16)
    nf = normed.astype(F32)
    in_pre = (
        jnp.sum(nf * w_igate_ref[...].astype(F32), axis=1, keepdims=True) + igate_bias_ref[...]
    )
    fpre = jnp.sum(nf * w_fgate_ref[...].astype(F32), axis=1, keepdims=True) + fgate_bias_ref[...]
    forget_log = jnp.minimum(fpre, 0.0) - jnp.log1p(jnp.exp(-jnp.abs(fpre)))
    carried = forget_log + column_of(log_scale_ref[...])
    new_max = jnp.maximum(carried, in_pre)
    carry_weight = jnp.exp(carried - new_max)
    fresh_weight = jnp.exp(in_pre - new_max)
    loads["query"].wait()
    query = jnp.dot(normed, w_query_v[...], preferred_element_type=F32) * key_dim ** (-0.5)
    loads["key"].wait()
    keys = jnp.dot(normed, w_key_v[...], preferred_element_type=F32)
    loads["value"].wait()
    values = jnp.dot(normed, w_value_v[...], preferred_element_type=F32)
    match = jnp.sum(query * keys, axis=1, keepdims=True)
    turned = query.T
    for i in range(pieces):
        memory_loads[i].wait()
        for s in range(i * piece, (i + 1) * piece):
            recall_v[s : s + 1, :] = jnp.sum(
                turned[:, s : s + 1] * memory_v[s], axis=0, keepdims=True
            )
    read = carry_weight * recall_v[...] + (fresh_weight * match) * values
    headout = (read * rms_scale(read) * head_gain_ref[...]).astype(BF16)
    loads["output"].wait()
    shares[0] = jnp.dot(headout, w_output_v[...], preferred_element_type=F32).astype(BF16)

    pl.semaphore_wait(barrier, groups * lanes - 1)
    copies = []
    for toff in range(1, lanes):
        copy = pltpu.make_async_remote_copy(
            src_ref=shares.at[0],
            dst_ref=shares.at[toff],
            send_sem=share_send.at[toff],
            recv_sem=share_recv.at[toff],
            device_id=device(0, toff),
            device_id_type=MESH,
        )
        copy.start()
        copies.append(copy)
    mine = [
        column_of(
            jnp.sum(
                jnp.where(
                    routes_ref[...] == lax.rem(ep + off, groups), route_weights_ref[...], 0.0
                ),
                axis=0,
                keepdims=True,
            )
        )
        for off in range(groups)
    ]
    mixed = shares[0].astype(F32)
    for toff in range(1, lanes):
        copies[toff - 1].wait_recv()
        mixed = mixed + shares[toff].astype(F32)
    resid = (xf + mixed * rms_scale(mixed) * gain_out_ref[...]).astype(BF16)
    rf = resid.astype(F32)
    rows[0] = (rf * rms_scale(rf) * ffn_gain_ref[...]).astype(BF16)
    for off in range(1, groups):
        copy = pltpu.make_async_remote_copy(
            src_ref=rows.at[0],
            dst_ref=rows.at[off],
            send_sem=rows_send.at[off],
            recv_sem=rows_recv.at[off],
            device_id=device(off, 0),
            device_id_type=MESH,
        )
        copy.start()
        copies.append(copy)
    for q in range(lanes):
        resid_v[q] = rf[:, q * quarter : (q + 1) * quarter]

    loads["gate"].wait()
    loads["up"].wait()
    loads["down"].wait()
    for copy in copies[lanes - 1 :]:
        copy.wait_recv()
    x = rows[...].reshape(groups * seqs, width)
    gate = jnp.dot(x, gate_v[...], preferred_element_type=F32)
    up = jnp.dot(x, up_v[...], preferred_element_type=F32)
    act = (jax.nn.silu(gate) * up).astype(BF16)
    for q in range(lanes):
        parts[q] = (
            jnp.dot(
                act, down_v[:, q * quarter : (q + 1) * quarter], preferred_element_type=F32
            )
            .astype(BF16)
            .reshape(groups, seqs, quarter)
        )
    back = {}
    for off in range(groups):
        for toff in range(lanes):
            src = parts.at[lax.rem(tp + toff, lanes), off]
            if off or toff:
                back[off, toff] = pltpu.make_async_remote_copy(
                    src_ref=src,
                    dst_ref=results.at[off, toff],
                    send_sem=parts_send.at[off, toff],
                    recv_sem=parts_recv.at[off, toff],
                    device_id=device(-off, toff),
                    device_id_type=MESH,
                )
                back[off, toff].start()

    routed = None
    for off in range(groups):
        total = None
        for toff in range(lanes):
            if off or toff:
                back[off, toff].wait_recv()
                part = results[off, toff]
            else:
                part = parts[tp, 0]
            part = part.astype(F32)
            total = part if total is None else total + part
        term = mine[off] * total.astype(BF16).astype(F32)
        routed = term if routed is None else routed + term
    squares[0] = jnp.broadcast_to(
        jnp.sum(routed * routed, axis=1, keepdims=True), squares.shape[1:]
    )
    last = []
    for toff in range(1, lanes):
        copy = pltpu.make_async_remote_copy(
            src_ref=squares.at[0],
            dst_ref=squares.at[toff],
            send_sem=squares_send.at[toff],
            recv_sem=squares_recv.at[toff],
            device_id=device(0, toff),
            device_id_type=MESH,
        )
        copy.start()
        last.append(copy)
    for copy in copies:
        copy.wait_send()
    for copy in back.values():
        copy.wait_send()
    total = squares[0]
    for toff in range(1, lanes):
        last[toff - 1].wait_recv()
        total = total + squares[toff]
    scaled = routed * lax.rsqrt(total[:, :1] / width + EPS)
    out_ref[...] = (resid_v[tp] + scaled * ffn_gain_out_ref[...]).astype(BF16)
    for copy in last:
        copy.wait_send()


def per_device(*args):
    (
        tokens,
        memory,
        log_scale,
        mix_gain_in,
        w_query,
        w_key,
        w_value,
        w_igate,
        w_fgate,
        igate_bias,
        fgate_bias,
        head_gain,
        w_output,
        mix_gain_out,
        ffn_gain_in,
        routes,
        route_weights,
        expert_gate,
        expert_up,
        expert_down,
        ffn_gain_out,
    ) = args
    groups = lax.axis_size("ep")
    lanes = lax.axis_size("tp")
    seqs, width = tokens.shape
    local_experts, _, hidden = expert_gate.shape
    top = routes.shape[1]
    if local_experts != 1 or log_scale.shape[1] != 1 or 2 * top < groups:
        return routed_device(*args)
    quarter = width // lanes
    key_dim, value_dim = memory.shape[2:]
    vmem = pl.BlockSpec(memory_space=pltpu.VMEM)
    hbm = pl.BlockSpec(memory_space=pl.ANY)
    dma = pltpu.SemaphoreType.DMA
    pieces = 4 if seqs % 4 == 0 else 1
    operands = (
        (tokens, hbm),
        (memory, hbm),
        (log_scale.T, vmem),
        (mix_gain_in.reshape(1, -1), vmem),
        (w_query, hbm),
        (w_key, hbm),
        (w_value, hbm),
        (w_igate.T, vmem),
        (w_fgate.T, vmem),
        (igate_bias.reshape(1, 1), vmem),
        (fgate_bias.reshape(1, 1), vmem),
        (head_gain.reshape(1, -1), vmem),
        (w_output, hbm),
        (mix_gain_out.reshape(1, -1), vmem),
        (ffn_gain_in.reshape(1, -1), vmem),
        (routes.T, vmem),
        (route_weights.T, vmem),
        (expert_gate, hbm),
        (expert_up, hbm),
        (expert_down, hbm),
        (ffn_gain_out.reshape(1, -1), vmem),
    )
    return pl.pallas_call(
        functools.partial(layer_kernel, groups, lanes),
        out_shape=jax.ShapeDtypeStruct((seqs, quarter), BF16),
        in_specs=[spec for _, spec in operands],
        out_specs=vmem,
        scratch_shapes=[
            pltpu.VMEM((seqs, width), BF16),
            pltpu.VMEM((seqs, key_dim, value_dim), F32),
            pltpu.VMEM(w_query.shape, BF16),
            pltpu.VMEM(w_key.shape, BF16),
            pltpu.VMEM(w_value.shape, BF16),
            pltpu.VMEM(w_output.shape, BF16),
            pltpu.VMEM((width, hidden), BF16),
            pltpu.VMEM((width, hidden), BF16),
            pltpu.VMEM((hidden, width), BF16),
            pltpu.VMEM((seqs, value_dim), F32),
            pltpu.VMEM((lanes, seqs, width), BF16),
            pltpu.VMEM((groups, seqs, width), BF16),
            pltpu.VMEM((lanes, seqs, quarter), F32),
            pltpu.VMEM((lanes, groups, seqs, quarter), BF16),
            pltpu.VMEM((groups, lanes, seqs, quarter), BF16),
            pltpu.VMEM((lanes, seqs, 128), F32),
            dma((8,)),
            dma((pieces,)),
            dma((lanes,)),
            dma((lanes,)),
            dma((groups,)),
            dma((groups,)),
            dma((groups, lanes)),
            dma((groups, lanes)),
            dma((lanes,)),
            dma((lanes,)),
        ],
        compiler_params=pltpu.CompilerParams(
            collective_id=0,
            has_side_effects=True,
            vmem_limit_bytes=60 * 1024 * 1024,
        ),
        name="layer",
    )(*[array for array, _ in operands])


def solution(mesh):
    return jax.shard_map(
        per_device,
        mesh=mesh,
        in_specs=(
            P("ep", None),
            P("ep", "tp", None, None),
            P("ep", "tp"),
            P(),
            P(None, "tp"),
            P(None, "tp"),
            P(None, "tp"),
            P(None, "tp"),
            P(None, "tp"),
            P("tp"),
            P("tp"),
            P("tp"),
            P("tp", None),
            P(),
            P(),
            P("ep", None),
            P("ep", None),
            P("ep", None, "tp"),
            P("ep", None, "tp"),
            P("ep", "tp", None),
            P("tp"),
        ),
        out_specs=P("ep", "tp"),
        check_vma=False,
    )
```

```python
import functools

import jax
import jax.numpy as jnp
from jax import lax
from jax.experimental import pallas as pl
from jax.experimental.pallas import tpu as pltpu
from jax.sharding import PartitionSpec as P

EPS = 1e-06


def rms_scale(values):
    return lax.rsqrt(jnp.mean(values * values, axis=-1, keepdims=True) + EPS)


def routed_device(
    tokens,
    memory,
    log_scale,
    mix_gain_in,
    w_query,
    w_key,
    w_value,
    w_igate,
    w_fgate,
    igate_bias,
    fgate_bias,
    head_gain,
    w_output,
    mix_gain_out,
    ffn_gain_in,
    routes,
    route_weights,
    expert_gate,
    expert_up,
    expert_down,
    ffn_gain_out,
):
    f32 = jnp.float32
    bf16 = jnp.bfloat16
    seqs, width = tokens.shape
    heads = log_scale.shape[1]
    key_dim = memory.shape[2]
    value_dim = memory.shape[3]
    xf = tokens.astype(f32)
    normed = (xf * rms_scale(xf) * mix_gain_in).astype(bf16)
    query = jnp.dot(normed, w_query, preferred_element_type=f32).reshape(
        seqs, heads, key_dim
    ) * key_dim ** (-0.5)
    keys = jnp.dot(normed, w_key, preferred_element_type=f32).reshape(seqs, heads, key_dim)
    values = jnp.dot(normed, w_value, preferred_element_type=f32).reshape(seqs, heads, value_dim)
    in_pre = jnp.dot(normed, w_igate, preferred_element_type=f32) + igate_bias
    forget_log = jax.nn.log_sigmoid(
        jnp.dot(normed, w_fgate, preferred_element_type=f32) + fgate_bias
    )
    carried = forget_log + log_scale
    new_max = jnp.maximum(carried, in_pre)
    carry_weight = jnp.exp(carried - new_max)
    fresh_weight = jnp.exp(in_pre - new_max)
    recall = jnp.einsum("shk,shkv->shv", query, memory, precision=lax.Precision.HIGHEST)
    match = jnp.sum(query * keys, axis=-1)
    read = carry_weight[..., None] * recall + (fresh_weight * match)[..., None] * values
    headout = (
        (read * rms_scale(read) * head_gain.reshape(heads, value_dim))
        .astype(bf16)
        .reshape(seqs, heads * value_dim)
    )
    partial_value = jnp.dot(headout, w_output, preferred_element_type=f32)
    mixed = lax.psum(partial_value.astype(jnp.bfloat16), "tp").astype(jnp.float32)
    resid = (xf + mixed * rms_scale(mixed) * mix_gain_out).astype(bf16)
    rf = resid.astype(f32)
    ffn_in = (rf * rms_scale(rf) * ffn_gain_in).astype(bf16)
    lanes = lax.axis_size("tp")
    quarter = width // lanes
    own = lax.axis_index("tp") * quarter
    local_experts = expert_gate.shape[0]
    experts_all = local_experts * lax.axis_size("ep")
    top = routes.shape[1]
    cap = min(seqs, max(2, 3 * seqs * top // (2 * experts_all)))
    flat = routes.reshape(-1)
    hits = (flat[:, None] == jnp.arange(experts_all, dtype=jnp.int32)[None, :]).astype(jnp.int32)
    earlier = jnp.cumsum(hits, axis=0) - hits
    slot = jnp.sum(earlier * hits, axis=1)
    place = (flat * cap + slot).reshape(seqs, top)
    picker = jnp.any(
        jnp.arange(experts_all * cap, dtype=jnp.int32)[:, None, None] == place[None, :, :], axis=2
    ).astype(bf16)
    outbound = (
        jnp.dot(picker, ffn_in, preferred_element_type=f32)
        .astype(bf16)
        .reshape(experts_all, cap, width)
    )
    arrived = lax.all_to_all(outbound, "ep", split_axis=0, concat_axis=0, tiled=True)
    items = arrived.shape[1]
    rows = arrived.reshape(-1, local_experts, items, width)
    gate = jnp.einsum("secd,edf->secf", rows, expert_gate, preferred_element_type=f32)
    up = jnp.einsum("secd,edf->secf", rows, expert_up, preferred_element_type=f32)
    act = (jax.nn.silu(gate) * up).astype(bf16)
    part = jnp.einsum("secf,efd->secd", act, expert_down, preferred_element_type=f32).reshape(
        -1, items, width
    )
    summed = lax.psum_scatter(
        part.astype(jnp.bfloat16), "tp", scatter_dimension=2, tiled=True
    ).astype(jnp.float32)
    done = summed.astype(bf16)
    returned = lax.all_to_all(done, "ep", split_axis=0, concat_axis=0, tiled=True)
    columns = returned.shape[2]
    chosen = jnp.take(returned.reshape(-1, columns), place.reshape(-1), axis=0).reshape(
        seqs, top, columns
    )
    routed = jnp.sum(route_weights[:, :, None] * chosen.astype(f32), axis=1)
    resid_part = lax.dynamic_slice_in_dim(rf, own, quarter, 1)
    total = lax.psum(jnp.sum(routed * routed, axis=1), "tp")
    scaled = routed * lax.rsqrt(total / width + EPS)[:, None]
    return (resid_part + scaled * ffn_gain_out).astype(bf16)


F32 = jnp.float32
BF16 = jnp.bfloat16
MESH = pl.DeviceIdType.MESH


def column_of(row):
    n = row.shape[1]
    eye = lax.broadcasted_iota(jnp.int32, (n, n), 0) == lax.broadcasted_iota(jnp.int32, (n, n), 1)
    return jnp.sum(jnp.where(eye, jnp.broadcast_to(row, (n, n)), 0.0), axis=1, keepdims=True)


def layer_kernel(
    groups,
    lanes,
    tokens_hbm,
    memory_hbm,
    log_scale_ref,
    gain_in_ref,
    w_query_hbm,
    w_key_hbm,
    w_value_hbm,
    w_igate_ref,
    w_fgate_ref,
    igate_bias_ref,
    fgate_bias_ref,
    head_gain_ref,
    w_output_hbm,
    gain_out_ref,
    ffn_gain_ref,
    routes_ref,
    route_weights_ref,
    gate_hbm,
    up_hbm,
    down_hbm,
    ffn_gain_out_ref,
    out_ref,
    tokens_v,
    memory_v,
    w_query_v,
    w_key_v,
    w_value_v,
    w_output_v,
    gate_v,
    up_v,
    down_v,
    recall_v,
    shares,
    rows,
    inbox,
    resid_v,
    parts,
    results,
    squares,
    load_sem,
    memory_sem,
    pair_send,
    pair_recv,
    share_send,
    share_recv,
    rows_send,
    rows_recv,
    parts_send,
    parts_recv,
    squares_send,
    squares_recv,
):
    ep = lax.axis_index("ep")
    tp = lax.axis_index("tp")
    seqs, width = tokens_v.shape
    key_dim = memory_v.shape[1]
    value_dim = memory_v.shape[2]
    quarter = width // lanes
    core, chip = lax.rem(tp, 2), tp // 2
    slots, chips, half = groups // 2, lanes // 2, width // 2

    def device(off, toff):
        return (lax.rem(ep + (off % groups), groups), lax.rem(tp + (toff % lanes), lanes))

    pieces = memory_sem.shape[0]
    piece = seqs // pieces
    loads = {}
    for i, (name, src, dst) in enumerate(
        (
            ("tokens", tokens_hbm, tokens_v),
            ("query", w_query_hbm, w_query_v),
            ("key", w_key_hbm, w_key_v),
            ("value", w_value_hbm, w_value_v),
            ("output", w_output_hbm, w_output_v),
            ("gate", gate_hbm.at[0], gate_v.at[0]),
            ("up", up_hbm.at[0], up_v.at[0]),
            ("down", down_hbm.at[0], down_v.at[0]),
        )
    ):
        loads[name] = pltpu.make_async_copy(src, dst, load_sem.at[i])
    memory_loads = [
        pltpu.make_async_copy(
            memory_hbm.at[pl.ds(i * piece, piece), 0],
            memory_v.at[pl.ds(i * piece, piece)],
            memory_sem.at[i],
        )
        for i in range(pieces)
    ]
    for name in ("tokens", "query", "key", "value"):
        loads[name].start()
    for load in memory_loads:
        load.start()
    for name in ("output", "gate", "up", "down"):
        loads[name].start()

    barrier = pltpu.get_barrier_semaphore()
    for off in range(groups):
        for toff in range(lanes):
            if off or toff:
                pl.semaphore_signal(
                    barrier, inc=1, device_id=device(off, toff), device_id_type=MESH
                )

    loads["tokens"].wait()
    xf = tokens_v[...].astype(F32)
    normed = (xf * rms_scale(xf) * gain_in_ref[...]).astype(BF16)
    nf = normed.astype(F32)
    in_pre = (
        jnp.sum(nf * w_igate_ref[...].astype(F32), axis=1, keepdims=True) + igate_bias_ref[...]
    )
    fpre = jnp.sum(nf * w_fgate_ref[...].astype(F32), axis=1, keepdims=True) + fgate_bias_ref[...]
    forget_log = jnp.minimum(fpre, 0.0) - jnp.log1p(jnp.exp(-jnp.abs(fpre)))
    carried = forget_log + column_of(log_scale_ref[...])
    new_max = jnp.maximum(carried, in_pre)
    carry_weight = jnp.exp(carried - new_max)
    fresh_weight = jnp.exp(in_pre - new_max)
    loads["query"].wait()
    query = jnp.dot(normed, w_query_v[...], preferred_element_type=F32) * key_dim ** (-0.5)
    loads["key"].wait()
    keys = jnp.dot(normed, w_key_v[...], preferred_element_type=F32)
    loads["value"].wait()
    values = jnp.dot(normed, w_value_v[...], preferred_element_type=F32)
    match = jnp.sum(query * keys, axis=1, keepdims=True)
    turned = query.T
    for i in range(pieces):
        memory_loads[i].wait()
        for s in range(i * piece, (i + 1) * piece):
            recall_v[s : s + 1, :] = jnp.sum(
                turned[:, s : s + 1] * memory_v[s], axis=0, keepdims=True
            )
    read = carry_weight * recall_v[...] + (fresh_weight * match) * values
    headout = (read * rms_scale(read) * head_gain_ref[...]).astype(BF16)
    loads["output"].wait()
    shares[0] = jnp.dot(headout, w_output_v[...], preferred_element_type=F32).astype(BF16)

    pl.semaphore_wait(barrier, groups * lanes - 1)
    copies = []
    for toff in range(1, lanes):
        copy = pltpu.make_async_remote_copy(
            src_ref=shares.at[0],
            dst_ref=shares.at[toff],
            send_sem=share_send.at[toff],
            recv_sem=share_recv.at[toff],
            device_id=device(0, toff),
            device_id_type=MESH,
        )
        copy.start()
        copies.append(copy)
    pairs = []
    for i, (name, ref) in enumerate((("gate", gate_v), ("up", up_v), ("down", down_v))):
        loads[name].wait()
        copy = pltpu.make_async_remote_copy(
            src_ref=ref.at[0],
            dst_ref=ref.at[1],
            send_sem=pair_send.at[i],
            recv_sem=pair_recv.at[i],
            device_id=(ep, tp + 1 - 2 * core),
            device_id_type=MESH,
        )
        copy.start()
        pairs.append(copy)
    mine = [
        column_of(
            jnp.sum(
                jnp.where(
                    routes_ref[...] == lax.rem(ep + off, groups), route_weights_ref[...], 0.0
                ),
                axis=0,
                keepdims=True,
            )
        )
        for off in range(groups)
    ]
    mixed = shares[0].astype(F32)
    for toff in range(1, lanes):
        copies[toff - 1].wait_recv()
        mixed = mixed + shares[toff].astype(F32)
    resid = (xf + mixed * rms_scale(mixed) * gain_out_ref[...]).astype(BF16)
    rf = resid.astype(F32)
    ffn_in = (rf * rms_scale(rf) * ffn_gain_ref[...]).astype(BF16)
    for h in range(2):
        rows[h] = ffn_in[:, h * half : (h + 1) * half]
    for off in range(groups - 1, 0, -1):
        copy = pltpu.make_async_remote_copy(
            src_ref=rows.at[core],
            dst_ref=inbox.at[core, off // 2],
            send_sem=rows_send.at[off],
            recv_sem=rows_recv.at[core, off // 2],
            device_id=(lax.rem(ep + off, groups), 2 * chip + off % 2),
            device_id_type=MESH,
        )
        copy.start()
        copies.append(copy)
    for q in range(lanes):
        resid_v[q] = rf[:, q * quarter : (q + 1) * quarter]

    def arrived(ref, sem):
        pltpu.make_async_copy(ref, ref, sem).wait()

    @pl.when(core == 0)
    def _():
        for h in range(2):
            inbox[h, 0] = ffn_in[:, h * half : (h + 1) * half]

    @pl.when(core == 1)
    def _():
        for h in range(2):
            arrived(inbox.at[h, 0], rows_recv.at[h, 0])

    for copy in pairs:
        copy.wait_recv()
    for slot in range(1, slots):
        for h in range(2):
            arrived(inbox.at[h, slot], rows_recv.at[h, slot])
    x = [inbox[h].reshape(slots * seqs, half) for h in range(2)]

    def into(weights, block):
        return sum(
            jnp.dot(
                x[h], weights[block, h * half : (h + 1) * half, :], preferred_element_type=F32
            )
            for h in range(2)
        )

    act = [
        (jax.nn.silu(into(gate_v, block)) * into(up_v, block)).astype(BF16) for block in range(2)
    ]
    for q in range(lanes):
        parts[q] = (
            sum(
                jnp.dot(
                    act[block],
                    down_v[block, :, q * quarter : (q + 1) * quarter],
                    preferred_element_type=F32,
                )
                for block in range(2)
            )
            .astype(BF16)
            .reshape(slots, seqs, quarter)
        )

    def result(slot, toff):
        return pltpu.make_async_remote_copy(
            src_ref=parts.at[lax.rem(tp + toff, lanes), slot],
            dst_ref=results.at[2 * slot + core, chip],
            send_sem=parts_send.at[slot, toff],
            recv_sem=parts_recv.at[2 * slot + core, chip],
            device_id=(
                lax.rem(ep + groups - 2 * slot - core, groups),
                lax.rem(tp + toff, lanes),
            ),
            device_id_type=MESH,
        )

    for slot in range(slots - 1, -1, -1):
        for toff in range(lanes - 1, -1, -1):
            if slot or toff:
                result(slot, toff).start()

    @pl.when(core == 1)
    def _():
        result(0, 0).start()

    @pl.when(core == 0)
    def _():
        results[0, chip] = parts[tp, 0]

    routed = None
    for off in range(groups):
        total = None
        for y in range(chips):
            if off:
                arrived(results.at[off, y], parts_recv.at[off, y])
            else:

                @pl.when((core == 1) | (chip != y))
                def _():
                    arrived(results.at[off, y], parts_recv.at[off, y])

            part = results[off, y].astype(F32)
            total = part if total is None else total + part
        term = mine[off] * total.astype(BF16).astype(F32)
        routed = term if routed is None else routed + term
    wide = squares.shape[2]
    eye = lax.broadcasted_iota(jnp.int32, (seqs, wide), 0) == lax.broadcasted_iota(
        jnp.int32, (seqs, wide), 1
    )
    squares[0] = jnp.sum(
        jnp.where(eye, jnp.sum(routed * routed, axis=1, keepdims=True), 0.0),
        axis=0,
        keepdims=True,
    )
    last = []
    for toff in range(1, lanes):
        copy = pltpu.make_async_remote_copy(
            src_ref=squares.at[0],
            dst_ref=squares.at[toff],
            send_sem=squares_send.at[toff],
            recv_sem=squares_recv.at[toff],
            device_id=device(0, toff),
            device_id_type=MESH,
        )
        copy.start()
        last.append(copy)
    for copy in copies:
        copy.wait_send()
    for copy in pairs:
        copy.wait_send()
    for slot in range(slots):
        for toff in range(lanes):
            if slot or toff:
                result(slot, toff).wait_send()

    @pl.when(core == 1)
    def _():
        result(0, 0).wait_send()

    total = squares[0]
    for toff in range(1, lanes):
        last[toff - 1].wait_recv()
        total = total + squares[toff]
    scale = jnp.sum(
        jnp.where(eye, lax.rsqrt(total / width + EPS), 0.0), axis=1, keepdims=True
    )
    scaled = routed * scale
    out_ref[...] = (resid_v[tp] + scaled * ffn_gain_out_ref[...]).astype(BF16)
    for copy in last:
        copy.wait_send()


def per_device(*args):
    (
        tokens,
        memory,
        log_scale,
        mix_gain_in,
        w_query,
        w_key,
        w_value,
        w_igate,
        w_fgate,
        igate_bias,
        fgate_bias,
        head_gain,
        w_output,
        mix_gain_out,
        ffn_gain_in,
        routes,
        route_weights,
        expert_gate,
        expert_up,
        expert_down,
        ffn_gain_out,
    ) = args
    groups = lax.axis_size("ep")
    lanes = lax.axis_size("tp")
    seqs, width = tokens.shape
    local_experts, _, hidden = expert_gate.shape
    top = routes.shape[1]
    if local_experts != 1 or log_scale.shape[1] != 1 or 2 * top < groups or groups % 2 or lanes % 2:
        return routed_device(*args)
    quarter = width // lanes
    key_dim, value_dim = memory.shape[2:]
    vmem = pl.BlockSpec(memory_space=pltpu.VMEM)
    hbm = pl.BlockSpec(memory_space=pl.ANY)
    dma = pltpu.SemaphoreType.DMA
    pieces = 4 if seqs % 4 == 0 else 1
    operands = (
        (tokens, hbm),
        (memory, hbm),
        (log_scale.T, vmem),
        (mix_gain_in.reshape(1, -1), vmem),
        (w_query, hbm),
        (w_key, hbm),
        (w_value, hbm),
        (w_igate.T, vmem),
        (w_fgate.T, vmem),
        (igate_bias.reshape(1, 1), vmem),
        (fgate_bias.reshape(1, 1), vmem),
        (head_gain.reshape(1, -1), vmem),
        (w_output, hbm),
        (mix_gain_out.reshape(1, -1), vmem),
        (ffn_gain_in.reshape(1, -1), vmem),
        (routes.T, vmem),
        (route_weights.T, vmem),
        (expert_gate, hbm),
        (expert_up, hbm),
        (expert_down, hbm),
        (ffn_gain_out.reshape(1, -1), vmem),
    )
    return pl.pallas_call(
        functools.partial(layer_kernel, groups, lanes),
        out_shape=jax.ShapeDtypeStruct((seqs, quarter), BF16),
        in_specs=[spec for _, spec in operands],
        out_specs=vmem,
        scratch_shapes=[
            pltpu.VMEM((seqs, width), BF16),
            pltpu.VMEM((seqs, key_dim, value_dim), F32),
            pltpu.VMEM(w_query.shape, BF16),
            pltpu.VMEM(w_key.shape, BF16),
            pltpu.VMEM(w_value.shape, BF16),
            pltpu.VMEM(w_output.shape, BF16),
            pltpu.VMEM((2, width, hidden), BF16),
            pltpu.VMEM((2, width, hidden), BF16),
            pltpu.VMEM((2, hidden, width), BF16),
            pltpu.VMEM((seqs, value_dim), F32),
            pltpu.VMEM((lanes, seqs, width), BF16),
            pltpu.VMEM((2, seqs, width // 2), BF16),
            pltpu.VMEM((2, groups // 2, seqs, width // 2), BF16),
            pltpu.VMEM((lanes, seqs, quarter), F32),
            pltpu.VMEM((lanes, groups // 2, seqs, quarter), BF16),
            pltpu.VMEM((groups, lanes // 2, seqs, quarter), BF16),
            pltpu.VMEM((lanes, 1, 128), F32),
            dma((8,)),
            dma((pieces,)),
            dma((3,)),
            dma((3,)),
            dma((lanes,)),
            dma((lanes,)),
            dma((groups,)),
            dma((2, groups // 2)),
            dma((groups // 2, lanes)),
            dma((groups, lanes // 2)),
            dma((lanes,)),
            dma((lanes,)),
        ],
        compiler_params=pltpu.CompilerParams(
            collective_id=0,
            has_side_effects=True,
            vmem_limit_bytes=60 * 1024 * 1024,
        ),
        name="layer",
    )(*[array for array, _ in operands])


def solution(mesh):
    return jax.shard_map(
        per_device,
        mesh=mesh,
        in_specs=(
            P("ep", None),
            P("ep", "tp", None, None),
            P("ep", "tp"),
            P(),
            P(None, "tp"),
            P(None, "tp"),
            P(None, "tp"),
            P(None, "tp"),
            P(None, "tp"),
            P("tp"),
            P("tp"),
            P("tp"),
            P("tp", None),
            P(),
            P(),
            P("ep", None),
            P("ep", None),
            P("ep", None, "tp"),
            P("ep", None, "tp"),
            P("ep", "tp", None),
            P("tp"),
        ),
        out_specs=P("ep", "tp"),
        check_vma=False,
    )
```

```python
import functools

import jax
import jax.numpy as jnp
from jax import lax
from jax.experimental import pallas as pl
from jax.experimental.pallas import tpu as pltpu
from jax.sharding import PartitionSpec as P

EPS = 1e-06


def rms_scale(values):
    return lax.rsqrt(jnp.mean(values * values, axis=-1, keepdims=True) + EPS)


def routed_device(
    tokens,
    memory,
    log_scale,
    mix_gain_in,
    w_query,
    w_key,
    w_value,
    w_igate,
    w_fgate,
    igate_bias,
    fgate_bias,
    head_gain,
    w_output,
    mix_gain_out,
    ffn_gain_in,
    routes,
    route_weights,
    expert_gate,
    expert_up,
    expert_down,
    ffn_gain_out,
):
    f32 = jnp.float32
    bf16 = jnp.bfloat16
    seqs, width = tokens.shape
    heads = log_scale.shape[1]
    key_dim = memory.shape[2]
    value_dim = memory.shape[3]
    xf = tokens.astype(f32)
    normed = (xf * rms_scale(xf) * mix_gain_in).astype(bf16)
    query = jnp.dot(normed, w_query, preferred_element_type=f32).reshape(
        seqs, heads, key_dim
    ) * key_dim ** (-0.5)
    keys = jnp.dot(normed, w_key, preferred_element_type=f32).reshape(seqs, heads, key_dim)
    values = jnp.dot(normed, w_value, preferred_element_type=f32).reshape(seqs, heads, value_dim)
    in_pre = jnp.dot(normed, w_igate, preferred_element_type=f32) + igate_bias
    forget_log = jax.nn.log_sigmoid(
        jnp.dot(normed, w_fgate, preferred_element_type=f32) + fgate_bias
    )
    carried = forget_log + log_scale
    new_max = jnp.maximum(carried, in_pre)
    carry_weight = jnp.exp(carried - new_max)
    fresh_weight = jnp.exp(in_pre - new_max)
    recall = jnp.einsum("shk,shkv->shv", query, memory, precision=lax.Precision.HIGHEST)
    match = jnp.sum(query * keys, axis=-1)
    read = carry_weight[..., None] * recall + (fresh_weight * match)[..., None] * values
    headout = (
        (read * rms_scale(read) * head_gain.reshape(heads, value_dim))
        .astype(bf16)
        .reshape(seqs, heads * value_dim)
    )
    partial_value = jnp.dot(headout, w_output, preferred_element_type=f32)
    mixed = lax.psum(partial_value.astype(jnp.bfloat16), "tp").astype(jnp.float32)
    resid = (xf + mixed * rms_scale(mixed) * mix_gain_out).astype(bf16)
    rf = resid.astype(f32)
    ffn_in = (rf * rms_scale(rf) * ffn_gain_in).astype(bf16)
    lanes = lax.axis_size("tp")
    quarter = width // lanes
    own = lax.axis_index("tp") * quarter
    local_experts = expert_gate.shape[0]
    experts_all = local_experts * lax.axis_size("ep")
    top = routes.shape[1]
    cap = min(seqs, max(2, 3 * seqs * top // (2 * experts_all)))
    flat = routes.reshape(-1)
    hits = (flat[:, None] == jnp.arange(experts_all, dtype=jnp.int32)[None, :]).astype(jnp.int32)
    earlier = jnp.cumsum(hits, axis=0) - hits
    slot = jnp.sum(earlier * hits, axis=1)
    place = (flat * cap + slot).reshape(seqs, top)
    picker = jnp.any(
        jnp.arange(experts_all * cap, dtype=jnp.int32)[:, None, None] == place[None, :, :], axis=2
    ).astype(bf16)
    outbound = (
        jnp.dot(picker, ffn_in, preferred_element_type=f32)
        .astype(bf16)
        .reshape(experts_all, cap, width)
    )
    arrived = lax.all_to_all(outbound, "ep", split_axis=0, concat_axis=0, tiled=True)
    items = arrived.shape[1]
    rows = arrived.reshape(-1, local_experts, items, width)
    gate = jnp.einsum("secd,edf->secf", rows, expert_gate, preferred_element_type=f32)
    up = jnp.einsum("secd,edf->secf", rows, expert_up, preferred_element_type=f32)
    act = (jax.nn.silu(gate) * up).astype(bf16)
    part = jnp.einsum("secf,efd->secd", act, expert_down, preferred_element_type=f32).reshape(
        -1, items, width
    )
    summed = lax.psum_scatter(
        part.astype(jnp.bfloat16), "tp", scatter_dimension=2, tiled=True
    ).astype(jnp.float32)
    done = summed.astype(bf16)
    returned = lax.all_to_all(done, "ep", split_axis=0, concat_axis=0, tiled=True)
    columns = returned.shape[2]
    chosen = jnp.take(returned.reshape(-1, columns), place.reshape(-1), axis=0).reshape(
        seqs, top, columns
    )
    routed = jnp.sum(route_weights[:, :, None] * chosen.astype(f32), axis=1)
    resid_part = lax.dynamic_slice_in_dim(rf, own, quarter, 1)
    total = lax.psum(jnp.sum(routed * routed, axis=1), "tp")
    scaled = routed * lax.rsqrt(total / width + EPS)[:, None]
    return (resid_part + scaled * ffn_gain_out).astype(bf16)


F32 = jnp.float32
BF16 = jnp.bfloat16
MESH = pl.DeviceIdType.MESH


def column_of(row):
    n = row.shape[1]
    eye = lax.broadcasted_iota(jnp.int32, (n, n), 0) == lax.broadcasted_iota(jnp.int32, (n, n), 1)
    return jnp.sum(jnp.where(eye, jnp.broadcast_to(row, (n, n)), 0.0), axis=1, keepdims=True)


def layer_kernel(
    groups,
    lanes,
    tokens_hbm,
    memory_hbm,
    log_scale_hbm,
    gain_in_hbm,
    w_query_hbm,
    w_key_hbm,
    w_value_hbm,
    w_igate_hbm,
    w_fgate_hbm,
    igate_bias_ref,
    fgate_bias_ref,
    head_gain_hbm,
    w_output_hbm,
    gain_out_hbm,
    ffn_gain_hbm,
    routes_hbm,
    route_weights_hbm,
    gate_hbm,
    up_hbm,
    down_hbm,
    ffn_gain_out_hbm,
    out_ref,
    log_scale_ref,
    gain_in_ref,
    w_igate_ref,
    w_fgate_ref,
    head_gain_ref,
    gain_out_ref,
    ffn_gain_ref,
    routes_ref,
    route_weights_ref,
    ffn_gain_out_ref,
    small_sem,
    tokens_v,
    memory_v,
    w_query_v,
    w_key_v,
    w_value_v,
    w_output_v,
    gate_v,
    up_v,
    down_v,
    recall_v,
    shares,
    rows,
    inbox,
    resid_v,
    parts,
    results,
    squares,
    load_sem,
    memory_sem,
    pair_send,
    pair_recv,
    share_send,
    share_recv,
    rows_send,
    rows_recv,
    parts_send,
    parts_recv,
    squares_send,
    squares_recv,
):
    ep = lax.axis_index("ep")
    tp = lax.axis_index("tp")
    seqs, width = tokens_v.shape
    key_dim = memory_v.shape[1]
    value_dim = memory_v.shape[2]
    quarter = width // lanes
    core, chip = lax.rem(tp, 2), tp // 2
    slots, chips, half = groups // 2, lanes // 2, width // 2

    def device(off, toff):
        return (lax.rem(ep + (off % groups), groups), lax.rem(tp + (toff % lanes), lanes))

    barrier = pltpu.get_barrier_semaphore()
    for off in range(groups):
        for toff in range(lanes):
            if off or toff:
                pl.semaphore_signal(
                    barrier, inc=1, device_id=device(off, toff), device_id_type=MESH
                )

    def partner(off):
        index, bit = 0, 1
        while bit < groups:
            index += bit * lax.rem(ep // bit + off // bit, 2)
            bit *= 2
        return index

    pieces = memory_sem.shape[0]
    piece = seqs // pieces
    loads = {}
    for i, (name, src, dst) in enumerate(
        (
            ("tokens", tokens_hbm, tokens_v),
            ("query", w_query_hbm, w_query_v),
            ("key", w_key_hbm, w_key_v),
            ("value", w_value_hbm, w_value_v),
            ("output", w_output_hbm, w_output_v),
            ("gate", gate_hbm.at[0], gate_v.at[0]),
            ("up", up_hbm.at[0], up_v.at[0]),
            ("down", down_hbm.at[0], down_v.at[0]),
        )
    ):
        loads[name] = pltpu.make_async_copy(src, dst, load_sem.at[i])
    memory_loads = [
        pltpu.make_async_copy(
            memory_hbm.at[pl.ds(i * piece, piece), 0],
            memory_v.at[pl.ds(i * piece, piece)],
            memory_sem.at[i],
        )
        for i in range(pieces)
    ]
    small = [
        pltpu.make_async_copy(src, dst, small_sem.at[i])
        for i, (src, dst) in enumerate(
            (
                (log_scale_hbm, log_scale_ref),
                (gain_in_hbm, gain_in_ref),
                (w_igate_hbm, w_igate_ref),
                (w_fgate_hbm, w_fgate_ref),
                (head_gain_hbm, head_gain_ref),
                (gain_out_hbm, gain_out_ref),
                (ffn_gain_hbm, ffn_gain_ref),
                (routes_hbm, routes_ref),
                (route_weights_hbm, route_weights_ref),
                (ffn_gain_out_hbm, ffn_gain_out_ref),
            )
        )
    ]
    loads["tokens"].start()
    for load in small:
        load.start()
    for name in ("query", "key", "value"):
        loads[name].start()
    for load in memory_loads:
        load.start()
    for name in ("output", "gate", "up", "down"):
        loads[name].start()

    loads["tokens"].wait()
    for load in small:
        load.wait()
    xf = tokens_v[...].astype(F32)
    normed = (xf * rms_scale(xf) * gain_in_ref[...]).astype(BF16)
    nf = normed.astype(F32)
    in_pre = (
        jnp.sum(nf * w_igate_ref[...].astype(F32), axis=1, keepdims=True) + igate_bias_ref[0]
    )
    fpre = jnp.sum(nf * w_fgate_ref[...].astype(F32), axis=1, keepdims=True) + fgate_bias_ref[0]
    forget_log = jnp.minimum(fpre, 0.0) - jnp.log1p(jnp.exp(-jnp.abs(fpre)))
    carried = forget_log + column_of(log_scale_ref[...])
    new_max = jnp.maximum(carried, in_pre)
    carry_weight = jnp.exp(carried - new_max)
    fresh_weight = jnp.exp(in_pre - new_max)
    loads["query"].wait()
    query = jnp.dot(normed, w_query_v[...], preferred_element_type=F32) * key_dim ** (-0.5)
    loads["key"].wait()
    keys = jnp.dot(normed, w_key_v[...], preferred_element_type=F32)
    loads["value"].wait()
    values = jnp.dot(normed, w_value_v[...], preferred_element_type=F32)
    match = jnp.sum(query * keys, axis=1, keepdims=True)
    turned = query.T
    for i in range(pieces):
        memory_loads[i].wait()
        for s in range(i * piece, (i + 1) * piece):
            recall_v[s : s + 1, :] = jnp.sum(
                turned[:, s : s + 1] * memory_v[s], axis=0, keepdims=True
            )
    read = carry_weight * recall_v[...] + (fresh_weight * match) * values
    headout = (read * rms_scale(read) * head_gain_ref[...]).astype(BF16)
    loads["output"].wait()
    shares[0] = jnp.dot(headout, w_output_v[...], preferred_element_type=F32).astype(BF16)

    pl.semaphore_wait(barrier, groups * lanes - 1)
    copies = []
    for toff in range(1, lanes):
        copy = pltpu.make_async_remote_copy(
            src_ref=shares.at[0],
            dst_ref=shares.at[toff],
            send_sem=share_send.at[toff],
            recv_sem=share_recv.at[toff],
            device_id=device(0, toff),
            device_id_type=MESH,
        )
        copy.start()
        copies.append(copy)
    pairs = []
    for i, (name, ref) in enumerate((("gate", gate_v), ("up", up_v), ("down", down_v))):
        loads[name].wait()
        copy = pltpu.make_async_remote_copy(
            src_ref=ref.at[0],
            dst_ref=ref.at[1],
            send_sem=pair_send.at[i],
            recv_sem=pair_recv.at[i],
            device_id=(ep, tp + 1 - 2 * core),
            device_id_type=MESH,
        )
        copy.start()
        pairs.append(copy)
    mine = [
        column_of(
            jnp.sum(
                jnp.where(
                    routes_ref[...] == partner(off), route_weights_ref[...], 0.0
                ),
                axis=0,
                keepdims=True,
            )
        )
        for off in range(groups)
    ]
    mixed = shares[0].astype(F32)
    for toff in range(1, lanes):
        copies[toff - 1].wait_recv()
        mixed = mixed + shares[toff].astype(F32)
    resid = (xf + mixed * rms_scale(mixed) * gain_out_ref[...]).astype(BF16)
    rf = resid.astype(F32)
    ffn_in = (rf * rms_scale(rf) * ffn_gain_ref[...]).astype(BF16)
    for h in range(2):
        rows[h] = ffn_in[:, h * half : (h + 1) * half]
    for off in range(1, groups):
        copy = pltpu.make_async_remote_copy(
            src_ref=rows.at[core],
            dst_ref=inbox.at[core, off // 2],
            send_sem=rows_send.at[off],
            recv_sem=rows_recv.at[core, off // 2],
            device_id=(partner(off), 2 * chip + off % 2),
            device_id_type=MESH,
        )
        copy.start()
        copies.append(copy)
    for q in range(lanes):
        resid_v[q] = rf[:, q * quarter : (q + 1) * quarter]

    def arrived(ref, sem):
        pltpu.make_async_copy(ref, ref, sem).wait()

    @pl.when(core == 0)
    def _():
        for h in range(2):
            inbox[h, 0] = ffn_in[:, h * half : (h + 1) * half]

    @pl.when(core == 1)
    def _():
        for h in range(2):
            arrived(inbox.at[h, 0], rows_recv.at[h, 0])

    for copy in pairs:
        copy.wait_recv()

    def result(slot, toff):
        group = partner(2 * slot) + core * (1 - 2 * lax.rem(ep, 2))
        return pltpu.make_async_remote_copy(
            src_ref=parts.at[lax.rem(tp + toff, lanes), slot],
            dst_ref=results.at[2 * slot + core, chip],
            send_sem=parts_send.at[slot, toff],
            recv_sem=parts_recv.at[2 * slot + core, chip],
            device_id=(group, lax.rem(tp + toff, lanes)),
            device_id_type=MESH,
        )

    for first, count in ((slot, 1) for slot in range(slots)):
        for slot in range(max(first, 1), first + count):
            for h in range(2):
                arrived(inbox.at[h, slot], rows_recv.at[h, slot])
        x = [inbox[h, first : first + count].reshape(count * seqs, half) for h in range(2)]

        def into(weights, block):
            return sum(
                jnp.dot(
                    x[h], weights[block, h * half : (h + 1) * half, :], preferred_element_type=F32
                )
                for h in range(2)
            )

        act = [
            (jax.nn.silu(into(gate_v, block)) * into(up_v, block)).astype(BF16)
            for block in range(2)
        ]
        for q in range(lanes):
            parts[q, first : first + count] = (
                sum(
                    jnp.dot(
                        act[block],
                        down_v[block, :, q * quarter : (q + 1) * quarter],
                        preferred_element_type=F32,
                    )
                    for block in range(2)
                )
                .astype(BF16)
                .reshape(count, seqs, quarter)
            )
        for slot in range(first, first + count):
            for toff in range(lanes - 1, -1, -1):
                if slot or toff:
                    result(slot, toff).start()
        if first == 0:

            @pl.when(core == 1)
            def _():
                result(0, 0).start()

            @pl.when(core == 0)
            def _():
                results[0, chip] = parts[tp, 0]

    routed = None
    for off in range(groups):
        total = None
        for y in range(chips):
            if off:
                arrived(results.at[off, y], parts_recv.at[off, y])
            else:

                @pl.when((core == 1) | (chip != y))
                def _():
                    arrived(results.at[off, y], parts_recv.at[off, y])

            part = results[off, y].astype(F32)
            total = part if total is None else total + part
        term = mine[off] * total.astype(BF16).astype(F32)
        routed = term if routed is None else routed + term
    wide = squares.shape[2]
    eye = lax.broadcasted_iota(jnp.int32, (seqs, wide), 0) == lax.broadcasted_iota(
        jnp.int32, (seqs, wide), 1
    )
    squares[0] = jnp.sum(
        jnp.where(eye, jnp.sum(routed * routed, axis=1, keepdims=True), 0.0),
        axis=0,
        keepdims=True,
    )
    last = []
    for toff in range(1, lanes):
        copy = pltpu.make_async_remote_copy(
            src_ref=squares.at[0],
            dst_ref=squares.at[toff],
            send_sem=squares_send.at[toff],
            recv_sem=squares_recv.at[toff],
            device_id=device(0, toff),
            device_id_type=MESH,
        )
        copy.start()
        last.append(copy)
    for copy in copies:
        copy.wait_send()
    for copy in pairs:
        copy.wait_send()
    for slot in range(slots):
        for toff in range(lanes):
            if slot or toff:
                result(slot, toff).wait_send()

    @pl.when(core == 1)
    def _():
        result(0, 0).wait_send()

    total = squares[0]
    for toff in range(1, lanes):
        last[toff - 1].wait_recv()
        total = total + squares[toff]
    scale = jnp.sum(
        jnp.where(eye, lax.rsqrt(total / width + EPS), 0.0), axis=1, keepdims=True
    )
    scaled = routed * scale
    out_ref[...] = (resid_v[tp] + scaled * ffn_gain_out_ref[...]).astype(BF16)
    for copy in last:
        copy.wait_send()


def per_device(*args):
    (
        tokens,
        memory,
        log_scale,
        mix_gain_in,
        w_query,
        w_key,
        w_value,
        w_igate,
        w_fgate,
        igate_bias,
        fgate_bias,
        head_gain,
        w_output,
        mix_gain_out,
        ffn_gain_in,
        routes,
        route_weights,
        expert_gate,
        expert_up,
        expert_down,
        ffn_gain_out,
    ) = args
    groups = lax.axis_size("ep")
    lanes = lax.axis_size("tp")
    seqs, width = tokens.shape
    local_experts, _, hidden = expert_gate.shape
    top = routes.shape[1]
    if local_experts != 1 or log_scale.shape[1] != 1 or 2 * top < groups or groups & (groups - 1) or groups < 4 or lanes % 2:
        return routed_device(*args)
    quarter = width // lanes
    key_dim, value_dim = memory.shape[2:]
    vmem = pl.BlockSpec(memory_space=pltpu.VMEM)
    hbm = pl.BlockSpec(memory_space=pl.ANY)
    smem = pl.BlockSpec(memory_space=pltpu.SMEM)
    dma = pltpu.SemaphoreType.DMA
    pieces = 4 if seqs % 4 == 0 else 1
    operands = (
        (tokens, hbm),
        (memory, hbm),
        (log_scale.T, hbm),
        (mix_gain_in.reshape(1, -1), hbm),
        (w_query, hbm),
        (w_key, hbm),
        (w_value, hbm),
        (w_igate.T, hbm),
        (w_fgate.T, hbm),
        (igate_bias, smem),
        (fgate_bias, smem),
        (head_gain.reshape(1, -1), hbm),
        (w_output, hbm),
        (mix_gain_out.reshape(1, -1), hbm),
        (ffn_gain_in.reshape(1, -1), hbm),
        (routes.T, hbm),
        (route_weights.T, hbm),
        (expert_gate, hbm),
        (expert_up, hbm),
        (expert_down, hbm),
        (ffn_gain_out.reshape(1, -1), hbm),
    )
    return pl.pallas_call(
        functools.partial(layer_kernel, groups, lanes),
        out_shape=pltpu.VMEM((seqs, quarter), BF16),
        in_specs=[spec for _, spec in operands],
        out_specs=vmem,
        scratch_shapes=[
            *[pltpu.VMEM(operands[i][0].shape, operands[i][0].dtype) for i in (2, 3, 7, 8, 11, 13, 14, 15, 16, 20)],
            dma((10,)),
            pltpu.VMEM((seqs, width), BF16),
            pltpu.VMEM((seqs, key_dim, value_dim), F32),
            pltpu.VMEM(w_query.shape, BF16),
            pltpu.VMEM(w_key.shape, BF16),
            pltpu.VMEM(w_value.shape, BF16),
            pltpu.VMEM(w_output.shape, BF16),
            pltpu.VMEM((2, width, hidden), BF16),
            pltpu.VMEM((2, width, hidden), BF16),
            pltpu.VMEM((2, hidden, width), BF16),
            pltpu.VMEM((seqs, value_dim), F32),
            pltpu.VMEM((lanes, seqs, width), BF16),
            pltpu.VMEM((2, seqs, width // 2), BF16),
            pltpu.VMEM((2, groups // 2, seqs, width // 2), BF16),
            pltpu.VMEM((lanes, seqs, quarter), F32),
            pltpu.VMEM((lanes, groups // 2, seqs, quarter), BF16),
            pltpu.VMEM((groups, lanes // 2, seqs, quarter), BF16),
            pltpu.VMEM((lanes, 1, 128), F32),
            dma((8,)),
            dma((pieces,)),
            dma((3,)),
            dma((3,)),
            dma((lanes,)),
            dma((lanes,)),
            dma((groups,)),
            dma((2, groups // 2)),
            dma((groups // 2, lanes)),
            dma((groups, lanes // 2)),
            dma((lanes,)),
            dma((lanes,)),
        ],
        compiler_params=pltpu.CompilerParams(
            collective_id=0,
            has_side_effects=True,
            vmem_limit_bytes=59 * 1024 * 1024,
        ),
        name="layer",
    )(*[array for array, _ in operands])


def solution(mesh):
    return jax.shard_map(
        per_device,
        mesh=mesh,
        in_specs=(
            P("ep", None),
            P("ep", "tp", None, None),
            P("ep", "tp"),
            P(),
            P(None, "tp"),
            P(None, "tp"),
            P(None, "tp"),
            P(None, "tp"),
            P(None, "tp"),
            P("tp"),
            P("tp"),
            P("tp"),
            P("tp", None),
            P(),
            P(),
            P("ep", None),
            P("ep", None),
            P("ep", None, "tp"),
            P("ep", None, "tp"),
            P("ep", "tp", None),
            P("tp"),
        ),
        out_specs=P("ep", "tp"),
        check_vma=False,
    )
```
